32 devices in a mesh: ep: 4 (over y, x), tp: 8 (over z, core).
Axes of the slice: x: 2, y: 2, z: 4, core: 2. Of those that a mesh axis runs over, the one named last changes fastest.
Arguments:
- query_rows: bfloat16 [512, 2048], P('ep', 'tp'), may hold values from -32 to 32
- key_rows: bfloat16 [512, 2048], P('ep', 'tp'), may hold values from -8 to 8
- value_rows: bfloat16 [512, 2048], P('ep', 'tp'), may hold values from -8 to 8
- query_norm_gain: float32 [64], replicated, may hold values from 0.1 to 1.9
- key_gain: float32 [64], replicated, may hold values from 0.1 to 1.9
- break_offset: float32 [32], P('tp'), may hold values from -12 to 3
- mixer_out_weight: bfloat16 [2048, 2048], P('tp'), may hold values from -0.75 to 0.75
- routed_tokens: bfloat16 [4096, 2048], P(('ep', 'tp')), may hold values from -6 to 6
- expert_gain: float32 [2048], replicated, may hold values from 0.1 to 1.9
- routes: int32 [4096, 2], P(('ep', 'tp')), may hold values from 0 to 3, as said below
- route_scores: float32 [4096, 2], P(('ep', 'tp')), may hold values from -6 to 6
- gate_weight: bfloat16 [4, 2048, 3584], P('ep', None, 'tp'), may hold values from -0.125 to 0.125
- up_weight: bfloat16 [4, 2048, 3584], P('ep', None, 'tp'), may hold values from -0.125 to 0.125
- down_weight: bfloat16 [4, 3584, 2048], P('ep', 'tp'), may hold values from -0.09375 to 0.09375
Outputs:
- attention_output: bfloat16 [512, 2048], P(('ep', 'tp'))
- expert_output: bfloat16 [4096, 2048], P(('ep', 'tp'))
The draws below stay inside these ranges and needn't reach their ends.
Inputs may be any that keep to these rules, and one draw needn't show every extreme that they name: `routes`: each row names 2 different experts. Among the rows of one device no expert is named more than 64 times, and one expert is named exactly 64 times by the rows of every device.
All inputs are finite; a program needn't handle non-finite values.
Results may differ from the reference program's by a relative error of at most 0.018.
Values may be sent and summed in bfloat16 or wider, within the bound.
A program may use at most 128 MiB of HBM per device.

```python
import math
import jax
import jax.numpy as jnp
from jax import lax

D = 2048
HEADS = 32
HEAD_DIM = 64
FFE = 3584
TOP_K = 2
TOK_DEV = 128
SEG = 128
SEQUENCE_TOKENS = 512
ROUTED = 4096
EXPERTS = 4
CAP = 64
N_TP = 8


def head_axes(key):
    sample = jax.random.normal(jax.random.fold_in(key, 101), (HEADS, HEAD_DIM), jnp.float32)
    return sample * lax.rsqrt(jnp.mean(sample * sample, axis=1, keepdims=True))


def draw_query_rows(key, part):
    direction = head_axes(key)
    jitter = jax.random.normal(jax.random.fold_in(key, 1), (SEQUENCE_TOKENS, HEADS, HEAD_DIM), jnp.float32)
    rows_out = jnp.clip(0.5 * jitter + direction[None], -32.0, 32.0)
    return rows_out.reshape(SEQUENCE_TOKENS, HEADS * HEAD_DIM).astype(jnp.bfloat16)


def draw_key_rows(key, part):
    direction = head_axes(key)
    blocks_count = SEQUENCE_TOKENS // SEG
    token_position = jnp.arange(SEQUENCE_TOKENS)
    jitter = jax.random.normal(jax.random.fold_in(key, 3), (SEQUENCE_TOKENS, HEADS, HEAD_DIM), jnp.float32)
    low_end = 0.4
    high_end = 1.6
    factor = jnp.exp(jax.random.uniform(jax.random.fold_in(key, 4), (blocks_count,), jnp.float32, jnp.log(low_end), jnp.log(high_end)))
    spread = jax.random.uniform(jax.random.fold_in(key, 5), (SEQUENCE_TOKENS, HEADS), jnp.float32, 0.6, 1.4)
    toward = -factor[token_position // SEG][:, None] * spread
    micro_batches = jax.random.randint(jax.random.fold_in(key, 6), (4,), 0, SEQUENCE_TOKENS)
    broken_stick = jnp.any(token_position[:, None] == micro_batches[None, :], axis=1)
    toward = jnp.where(broken_stick[:, None], 0.2, toward)
    rows_out = jnp.clip(0.5 * jitter + toward[:, :, None] * direction[None], -8.0, 8.0)
    return rows_out.reshape(SEQUENCE_TOKENS, HEADS * HEAD_DIM).astype(jnp.bfloat16)


def draw_value_rows(key, part):
    blocks_count = SEQUENCE_TOKENS // SEG
    levels = jax.random.uniform(jax.random.fold_in(key, 7), (blocks_count, HEADS * HEAD_DIM), jnp.float32, -1.5, 1.5)
    jitter = jax.random.normal(jax.random.fold_in(key, 8), (SEQUENCE_TOKENS, HEADS * HEAD_DIM), jnp.float32)
    rows_out = jnp.clip(jitter + jnp.repeat(levels, SEG, axis=0), -8.0, 8.0)
    return rows_out.astype(jnp.bfloat16)


def draw_break_offset(key, part):
    quick_share = 0.5
    quick = jax.random.uniform(jax.random.fold_in(key, 9), (HEADS,), jnp.float32) < quick_share
    quick_value = jax.random.uniform(jax.random.fold_in(key, 10), (HEADS,), jnp.float32, 2.0, 3.0)
    slow_value = jax.random.uniform(jax.random.fold_in(key, 11), (HEADS,), jnp.float32, 5.0, 6.0) - jnp.log(SEQUENCE_TOKENS * 1.0)
    return jnp.where(quick, quick_value, slow_value).astype(jnp.float32)


def draw_routes(key, part):
    blocks_count = ROUTED // TOK_DEV

    def one_block(block_key):
        reserve = jnp.tile(jnp.arange(1, EXPERTS, dtype=jnp.int32), CAP)
        reserve = jax.random.permutation(jax.random.fold_in(block_key, 1), reserve)
        remainder = jnp.sort(reserve[:TOK_DEV * TOP_K - CAP])
        ordered = jnp.concatenate([jnp.zeros((CAP,), jnp.int32), remainder])
        paired = ordered.reshape(TOP_K, TOK_DEV).T
        shuffle = jax.random.permutation(jax.random.fold_in(block_key, 2), TOK_DEV)
        labels = jax.random.permutation(jax.random.fold_in(block_key, 3), EXPERTS).astype(jnp.int32)
        return labels[paired[shuffle]]
    block_keys = jax.random.split(jax.random.fold_in(key, 13), blocks_count)
    chosen = jax.vmap(one_block)(block_keys).reshape(ROUTED, TOP_K)
    return chosen.astype(jnp.int32)


def block_scale(rng, extent, shards, low, largest):
    factor_of, own = 1.0, jax.random.fold_in(rng, 6)
    for position, parts in shards:
        heights = jnp.exp(jax.random.uniform(jax.random.fold_in(own, position), (parts,), jnp.float32, low / len(shards), largest / len(shards)))
        factor_of = factor_of * jnp.repeat(heights, extent[position] // parts).reshape([-1 if axis == position else 1 for axis in range(len(extent))])
    return factor_of


def noise(rng, dims, deviation, reach, cuts=(), held_as=jnp.bfloat16):
    values = jax.random.normal(rng, dims, jnp.float32) * deviation
    if len(cuts) > 0:
        values = block_scale(rng, dims, cuts, -0.22, 0.18) * values
    return jnp.clip(values, min=-reach, max=reach).astype(held_as)


def setup_inputs(seed: int = 0) -> dict:
    key_list = jax.random.split(jax.random.key(seed), 15)
    return {
        "query_rows": draw_query_rows(jax.random.fold_in(key_list[14], 71), 0),
        "key_rows": draw_key_rows(jax.random.fold_in(key_list[14], 71), 0),
        "value_rows": draw_value_rows(jax.random.fold_in(key_list[14], 71), 0),
        "query_norm_gain": jnp.clip(1.0 + 0.18 * jax.random.normal(key_list[3], (HEAD_DIM,), jnp.float32), 0.1, 1.9),
        "key_gain": jnp.clip(1.0 + 0.18 * jax.random.normal(key_list[4], (HEAD_DIM,), jnp.float32), 0.1, 1.9),
        "break_offset": draw_break_offset(jax.random.fold_in(key_list[14], 71), 0),
        "mixer_out_weight": noise(key_list[6], (HEADS * HEAD_DIM, D), HEAD_DIM ** -0.5, 0.75, ((0, 8),)),
        "routed_tokens": noise(key_list[7], (ROUTED, D), 1.0, 6.0, ((0, 32),)),
        "expert_gain": jnp.clip(1.0 + 0.18 * jax.random.normal(key_list[8], (D,), jnp.float32), 0.1, 1.9),
        "routes": draw_routes(jax.random.fold_in(key_list[14], 71), 0),
        "route_scores": noise(key_list[10], (ROUTED, TOP_K), 1.5, 6.0, ((0, 32),), jnp.float32),
        "gate_weight": noise(key_list[11], (EXPERTS, D, FFE), D ** -0.5, 0.125, ((0, 4), (2, 8))),
        "up_weight": noise(key_list[12], (EXPERTS, D, FFE), D ** -0.5, 0.125, ((0, 4), (2, 8))),
        "down_weight": noise(key_list[13], (EXPERTS, FFE, D), FFE ** -0.5, 0.09375, ((0, 4), (1, 8))),
    }


EPS = 1e-06

def norm_heads(flat, gain):
    count = flat.shape[0]
    split = flat.astype(jnp.float32).reshape(count, -1, HEAD_DIM)
    scaled = split * lax.rsqrt(lax.optimization_barrier(jnp.mean(split * split, axis=2, keepdims=True)) + EPS)
    return (scaled * gain).astype(jnp.bfloat16)

def attention_part(query_rows, key_rows, value_rows, query_norm_gain, key_gain, break_offset, mixer_out_weight):
    length = query_rows.shape[0]
    query_norm = norm_heads(query_rows, query_norm_gain)
    key_norm = norm_heads(key_rows, key_gain)
    value_heads = value_rows.reshape(length, HEADS, HEAD_DIM)
    block_size = math.gcd(512, length)
    gathered = []
    for block_start in range(0, length, block_size):
        block_end = block_start + block_size
        query_place = block_start + jnp.arange(block_size, dtype=jnp.int32)[:, None]
        key_place = jnp.arange(block_end, dtype=jnp.int32)[None, :]
        before = key_place < query_place

        def one_head(inputs):
            query_head, key_head, value_head, offset_value = inputs
            scores = jnp.dot(query_head, key_head.T, preferred_element_type=jnp.float32) * HEAD_DIM ** (-0.5) + offset_value
            log_rise = jax.nn.log_sigmoid(scores)
            log_fail = jnp.where(before, log_rise - scores, 0.0)
            log_after = lax.cumsum(log_fail, axis=1, reverse=True) - log_fail
            weights = jnp.where(before, jnp.exp(log_rise + log_after), 0.0).astype(jnp.bfloat16)
            return jnp.dot(weights, value_head, preferred_element_type=jnp.float32).astype(jnp.bfloat16)
        heads_out = lax.map(one_head, (jnp.moveaxis(query_norm[block_start:block_end], 1, 0), jnp.moveaxis(key_norm[:block_end], 1, 0), jnp.moveaxis(value_heads[:block_end], 1, 0), break_offset))
        gathered.append(jnp.moveaxis(heads_out, 0, 1).reshape(block_size, HEADS * HEAD_DIM))
    heads_mixed = jnp.concatenate(gathered, axis=0)
    group_width = HEADS * HEAD_DIM // N_TP
    running_sum = jnp.zeros((length, D), jnp.float32)
    for group_index in range(N_TP):
        low_edge = group_index * group_width
        term = jnp.dot(heads_mixed[:, low_edge:low_edge + group_width], mixer_out_weight[low_edge:low_edge + group_width], preferred_element_type=jnp.float32).astype(jnp.bfloat16)
        running_sum = running_sum + term.astype(jnp.float32)
    return running_sum.astype(jnp.bfloat16)

def expert_part(routed_tokens, expert_gain, routes, route_scores, gate_weight, up_weight, down_weight):
    row_count = routed_tokens.shape[0]
    as_float = routed_tokens.astype(jnp.float32)
    normed = (as_float * lax.rsqrt(lax.optimization_barrier(jnp.mean(as_float * as_float, axis=1, keepdims=True)) + EPS) * expert_gain).astype(jnp.bfloat16)
    differences = route_scores[:, None, :] - route_scores[:, :, None]
    route_weight = 1.0 / lax.optimization_barrier(jnp.sum(jnp.exp(differences), axis=2))
    flat_routes = routes.reshape(-1).astype(jnp.int32)
    copy_count = flat_routes.shape[0]
    block_count = row_count // TOK_DEV
    member = (flat_routes[:, None] == jnp.arange(EXPERTS, dtype=jnp.int32)[None, :]).astype(jnp.int32)
    member = member.reshape(block_count, TOK_DEV * TOP_K, EXPERTS)
    ahead = lax.optimization_barrier(jnp.sum((jnp.cumsum(member, axis=1) - member) * member, axis=2)).reshape(-1)
    owner = jnp.arange(copy_count, dtype=jnp.int32) // (TOK_DEV * TOP_K)
    slot_index = (owner * CAP + ahead).astype(jnp.int32)
    sources = jnp.repeat(normed, TOP_K, axis=0)
    room = block_count * CAP
    unit_width = FFE // N_TP

    def single_expert(carry, expert_index):
        chosen = flat_routes == expert_index
        target = jnp.where(chosen, slot_index, room).astype(jnp.int32)
        rows_in = jnp.zeros((room, D), jnp.bfloat16).at[target].set(sources, mode='drop')
        gate_part = jnp.dot(rows_in, gate_weight[expert_index], preferred_element_type=jnp.float32)
        up_part = jnp.dot(rows_in, up_weight[expert_index], preferred_element_type=jnp.float32)
        hidden = (jax.nn.silu(gate_part) * up_part).astype(jnp.bfloat16)
        down_here = down_weight[expert_index]
        running_sum = jnp.zeros((room, D), jnp.float32)
        for unit_index in range(N_TP):
            low_edge = unit_index * unit_width
            term = jnp.dot(hidden[:, low_edge:low_edge + unit_width], down_here[low_edge:low_edge + unit_width], preferred_element_type=jnp.float32).astype(jnp.bfloat16)
            running_sum = running_sum + term.astype(jnp.float32)
        result = running_sum.astype(jnp.bfloat16)
        picked = result[jnp.minimum(target, room - 1)]
        return (jnp.where(chosen[:, None], picked.astype(jnp.float32), carry), None)
    results, _ = lax.scan(single_expert, jnp.zeros((copy_count, D), jnp.float32), jnp.arange(EXPERTS, dtype=jnp.int32))
    results = results.reshape(row_count, TOP_K, D)
    return lax.optimization_barrier(jnp.sum(route_weight[..., None] * results, axis=1)).astype(jnp.bfloat16)

def reference(query_rows, key_rows, value_rows, query_norm_gain, key_gain, break_offset, mixer_out_weight, routed_tokens, expert_gain, routes, route_scores, gate_weight, up_weight, down_weight):
    attention_output = attention_part(query_rows, key_rows, value_rows, query_norm_gain, key_gain, break_offset, mixer_out_weight)
    expert_output = expert_part(routed_tokens, expert_gain, routes, route_scores, gate_weight, up_weight, down_weight)
    return (attention_output, expert_output)
```

```python
import jax
import jax.numpy as jnp
from jax import lax
from jax.sharding import PartitionSpec as P

HEAD_DIM = 64
TOP_K = 2


EPS = 1e-06
TAGS = 128


def norm_heads(flat, gain):
    count = flat.shape[0]
    split = flat.astype(jnp.float32).reshape(count, -1, HEAD_DIM)
    scaled = split * lax.rsqrt(jnp.mean(split * split, axis=2, keepdims=True) + EPS)
    return (scaled * gain).astype(jnp.bfloat16)


def swap_cores(array):
    pairs = [(i, i ^ 1) for i in range(lax.axis_size("tp"))]
    return lax.ppermute(array, "tp", pairs)


def to_distance(array, distance):
    pairs = [(i, i ^ distance) for i in range(lax.axis_size("ep"))]
    return lax.ppermute(array, "ep", pairs)


def along_tp(array, step):
    size = lax.axis_size("tp")
    pairs = [(i, (i + 2 * step) % size) for i in range(size)]
    return lax.ppermute(array, "tp", pairs)


def gather_chips(array):
    blocks = [array]
    for _ in range(1, lax.axis_size("tp") // 2):
        blocks.append(along_tp(blocks[-1], 1))
    return jnp.stack(blocks)


def scatter_chips(blocks):
    total = blocks[-1]
    for d in reversed(range(lax.axis_size("tp") // 2 - 1)):
        moved = along_tp(total, -1).astype(jnp.float32)
        total = (moved + blocks[d].astype(jnp.float32)).astype(jnp.bfloat16)
    return total


def attention(query_rows, key_rows, value_rows, query_norm_gain, key_gain, break_offset):
    row_count, width = query_rows.shape
    query_norm = norm_heads(query_rows, query_norm_gain)
    key_flat = norm_heads(key_rows, key_gain).reshape(row_count, width)
    both = lax.all_gather(
        jnp.concatenate([key_flat, value_rows], axis=1), "ep", axis=0, tiled=True
    )
    length = both.shape[0]
    key_norm = both[:, :width].reshape(length, -1, HEAD_DIM)
    value_heads = both[:, width:].reshape(length, -1, HEAD_DIM)
    query_place = lax.axis_index("ep") * row_count + jnp.arange(row_count)
    key_place = jnp.arange(length)
    allowed = (key_place[None, :] < query_place[:, None])[None]
    scores = jnp.einsum("qhd,khd->hqk", query_norm, key_norm, preferred_element_type=jnp.float32)
    scores = scores * HEAD_DIM ** (-0.5) + break_offset[:, None, None]
    log_rise = jax.nn.log_sigmoid(scores)
    log_fail = jnp.where(allowed, log_rise - scores, 0.0)
    later = (key_place[:, None] > key_place[None, :]).astype(jnp.float32)
    log_after = jnp.einsum(
        "hqj,jk->hqk",
        log_fail,
        later,
        precision=lax.Precision.HIGHEST,
        preferred_element_type=jnp.float32,
    )
    weights = jnp.where(allowed, jnp.exp(log_rise + log_after), 0.0).astype(jnp.bfloat16)
    mixed = jnp.einsum("hqk,khd->qhd", weights, value_heads, preferred_element_type=jnp.float32)
    return mixed.astype(jnp.bfloat16).reshape(row_count, width)


def body(
    query_rows,
    key_rows,
    value_rows,
    query_norm_gain,
    key_gain,
    break_offset,
    mixer_out_weight,
    routed_tokens,
    expert_gain,
    routes,
    route_scores,
    gate_weight,
    up_weight,
    down_weight,
):
    f32, bf16 = jnp.float32, jnp.bfloat16
    experts = lax.axis_size("ep")
    chips = lax.axis_size("tp") // 2
    my_ep = lax.axis_index("ep")
    core = lax.axis_index("tp") % 2
    count, width = routed_tokens.shape
    half = width // 2
    capacity = count * TOP_K // experts
    slots = experts * capacity

    gates = (gate_weight[0], swap_cores(gate_weight[0]))
    ups = (up_weight[0], swap_cores(up_weight[0]))
    downs = (down_weight[0], swap_cores(down_weight[0]))
    mixers = (mixer_out_weight, swap_cores(mixer_out_weight))

    as_float = routed_tokens.astype(f32)
    normed = (
        as_float
        * lax.rsqrt(jnp.mean(as_float * as_float, axis=1, keepdims=True) + EPS)
        * expert_gain
    ).astype(bf16)
    differences = route_scores[:, None, :] - route_scores[:, :, None]
    route_weight = 1.0 / jnp.sum(jnp.exp(differences), axis=2)

    away = jnp.bitwise_xor(routes, my_ep)
    flat = away.reshape(-1)
    member = (flat[:, None] == jnp.arange(experts, dtype=jnp.int32)[None, :]).astype(bf16)
    earlier = jnp.arange(flat.shape[0])
    earlier = (earlier[None, :] < earlier[:, None]).astype(bf16)
    rank = jnp.dot(earlier, member, preferred_element_type=f32)
    ahead = jnp.sum(rank * member.astype(f32), axis=1).reshape(count, TOP_K)

    weight_high = lax.reduce_precision(route_weight, 8, 7)
    weight_mid = lax.reduce_precision(route_weight - weight_high, 8, 7)
    weight_low = route_weight - weight_high - weight_mid
    tags = jnp.concatenate(
        [away.astype(f32), ahead, weight_high, weight_mid, weight_low], axis=1
    ).astype(bf16)
    tags = jnp.pad(tags, ((0, 0), (0, TAGS - tags.shape[1])))
    tokens = gather_chips(jnp.concatenate([normed[:, half:], tags], axis=1))

    slot_list = jnp.arange(slots, dtype=f32)

    def selection(away_of, ahead_of):
        slot_index = away_of.astype(f32) * capacity + ahead_of
        return (slot_index[..., None] == slot_list).astype(bf16)

    select = selection(away, ahead)
    outgoing = jnp.einsum(
        "ns,nd->sd", jnp.sum(select, axis=1), normed[:, :half], preferred_element_type=f32
    ).astype(bf16).reshape(experts, capacity, half)
    arrived = jnp.stack(
        [outgoing[0]] + [to_distance(outgoing[s], s) for s in range(1, experts)]
    )
    first = gather_chips(arrived).reshape(-1, half)

    away_all = tokens[:, :, half : half + 2].astype(f32)
    ahead_all = tokens[:, :, half + 2 : half + 4].astype(f32)
    weight_all = (
        tokens[:, :, half + 4 : half + 6].astype(f32)
        + tokens[:, :, half + 6 : half + 8].astype(f32)
        + tokens[:, :, half + 8 : half + 10].astype(f32)
    )
    select_all = selection(away_all, ahead_all)
    spread = jnp.einsum(
        "tns,tnd->tsd",
        jnp.sum(select_all, axis=2),
        tokens[:, :, :half],
        preferred_element_type=f32,
    ).astype(bf16).reshape(chips, experts, capacity, half)
    second = jnp.stack(
        [spread[:, 0]] + [to_distance(spread[:, s], s) for s in range(1, experts)], axis=1
    ).reshape(-1, half)

    heads_mixed = attention(
        query_rows, key_rows, value_rows, query_norm_gain, key_gain, break_offset
    )
    rows = heads_mixed.shape[0] // (2 * chips)
    my_chip = lax.axis_index("tp") // 2
    by_chip = heads_mixed.reshape(chips, 2, rows, -1)
    by_core = jnp.stack(
        [lax.dynamic_index_in_dim(by_chip, (my_chip - d) % chips, 0, keepdims=False) for d in range(chips)]
    )
    mine = lax.dynamic_index_in_dim(by_core, core, 1, keepdims=False)
    theirs = lax.dynamic_index_in_dim(by_core, 1 - core, 1, keepdims=False)
    other = swap_cores(theirs)
    mixer_terms = jnp.dot(
        mine.reshape(chips * rows, -1), mixers[0], preferred_element_type=f32
    ) + jnp.dot(other.reshape(chips * rows, -1), mixers[1], preferred_element_type=f32)
    mixer_terms = mixer_terms.astype(bf16).reshape(chips, 2 * rows, half)

    hidden = []
    for gate, up in zip(gates, ups):
        gate_piece = jnp.dot(first, gate[:half], preferred_element_type=f32) + jnp.dot(
            second, gate[half:], preferred_element_type=f32
        )
        up_piece = jnp.dot(first, up[:half], preferred_element_type=f32) + jnp.dot(
            second, up[half:], preferred_element_type=f32
        )
        hidden.append((jax.nn.silu(gate_piece) * up_piece).astype(bf16))

    def down_terms(columns):
        return (
            jnp.dot(hidden[0], downs[0][:, columns], preferred_element_type=f32)
            + jnp.dot(hidden[1], downs[1][:, columns], preferred_element_type=f32)
        ).astype(bf16).reshape(chips, experts, capacity, half)

    second_terms = down_terms(slice(half, width))
    first_terms = down_terms(slice(0, half))
    first_terms, second_terms = lax.optimization_barrier((first_terms, second_terms))

    first_sum = scatter_chips(first_terms)
    second_back = jnp.stack(
        [second_terms[:, 0]] + [to_distance(second_terms[:, s], s) for s in range(1, experts)],
        axis=1,
    ).reshape(chips, slots, half)
    picked = jnp.einsum(
        "tnks,tsd->tknd", select_all, second_back, preferred_element_type=f32
    )
    second_mix = jnp.sum(
        jnp.swapaxes(weight_all, 1, 2)[..., None] * picked, axis=1
    ).astype(bf16)
    last_sum = scatter_chips(jnp.concatenate([second_mix, mixer_terms], axis=1))
    first_back = jnp.stack(
        [first_sum[0]] + [to_distance(first_sum[s], s) for s in range(1, experts)]
    ).reshape(slots, half)
    first_picked = jnp.einsum("nks,sd->knd", select, first_back, preferred_element_type=f32)
    first_out = jnp.sum(route_weight.T[..., None] * first_picked, axis=0).astype(bf16)
    expert_output = jnp.concatenate([first_out, last_sum[:count]], axis=1)
    return (last_sum[count:].reshape(rows, width), expert_output)


def solution(mesh):
    in_specs = (
        P("ep", "tp"),
        P("ep", "tp"),
        P("ep", "tp"),
        P(),
        P(),
        P("tp"),
        P("tp", None),
        P(("ep", "tp"), None),
        P(),
        P(("ep", "tp"), None),
        P(("ep", "tp"), None),
        P("ep", None, "tp"),
        P("ep", None, "tp"),
        P("ep", "tp", None),
    )
    out_specs = (P(("ep", "tp"), None), P(("ep", "tp"), None))
    return jax.shard_map(body, mesh=mesh, in_specs=in_specs, out_specs=out_specs, check_vma=False)
```

```python
import jax
import jax.numpy as jnp
from jax import lax
from jax.sharding import PartitionSpec as P

HEAD_DIM = 64
TOP_K = 2


EPS = 1e-06
TAGS = 128


def norm_heads(flat, gain):
    count = flat.shape[0]
    split = flat.astype(jnp.float32).reshape(count, -1, HEAD_DIM)
    scaled = split * lax.rsqrt(jnp.mean(split * split, axis=2, keepdims=True) + EPS)
    return (scaled * gain).astype(jnp.bfloat16)


def swap_cores(array):
    pairs = [(i, i ^ 1) for i in range(lax.axis_size("tp"))]
    return lax.ppermute(array, "tp", pairs)


def to_distance(array, distance):
    pairs = [(i, i ^ distance) for i in range(lax.axis_size("ep"))]
    return lax.ppermute(array, "ep", pairs)


def along_tp(array, step):
    size = lax.axis_size("tp")
    pairs = [(i, (i + 2 * step) % size) for i in range(size)]
    return lax.ppermute(array, "tp", pairs)


def gather_chips(array):
    blocks = [array]
    for _ in range(1, lax.axis_size("tp") // 2):
        blocks.append(along_tp(blocks[-1], 1))
    return jnp.stack(blocks)


def scatter_chips(blocks):
    last = lax.axis_size("tp") // 2 - 1
    total = blocks[last]
    for step in range(1, last + 1):
        moved = along_tp(total, -1)
        total = moved.astype(jnp.float32) + blocks[last - step].astype(jnp.float32)
        total = total.astype(jnp.bfloat16)
    return total


def attention(query_rows, key_rows, value_rows, query_norm_gain, key_gain, break_offset):
    row_count, width = query_rows.shape
    query_norm = norm_heads(query_rows, query_norm_gain)
    key_flat = norm_heads(key_rows, key_gain).reshape(row_count, width)
    own = jnp.concatenate([key_flat, value_rows], axis=1)
    parts = lax.axis_size("ep")
    both = jnp.concatenate([own] + [to_distance(own, d) for d in range(1, parts)])
    length = both.shape[0]
    key_norm = both[:, :width].reshape(length, -1, HEAD_DIM)
    value_heads = both[:, width:].reshape(length, -1, HEAD_DIM)
    my_index = lax.axis_index("ep")
    query_place = my_index * row_count + jnp.arange(row_count)
    key_owner = jnp.bitwise_xor(jnp.arange(parts), my_index)
    key_place = (key_owner[:, None] * row_count + jnp.arange(row_count)).reshape(-1)
    allowed = (key_place[None, :] < query_place[:, None])[None]
    scores = jnp.einsum("qhd,khd->hqk", query_norm, key_norm, preferred_element_type=jnp.float32)
    scores = scores * HEAD_DIM ** (-0.5) + break_offset[:, None, None]
    log_rise = jax.nn.log_sigmoid(scores)
    log_fail = jnp.where(allowed, log_rise - scores, 0.0)
    later = (key_place[:, None] > key_place[None, :]).astype(jnp.float32)
    log_after = jnp.einsum(
        "hqj,jk->hqk",
        log_fail,
        later,
        precision=lax.Precision.HIGHEST,
        preferred_element_type=jnp.float32,
    )
    weights = jnp.where(allowed, jnp.exp(log_rise + log_after), 0.0).astype(jnp.bfloat16)
    mixed = jnp.einsum("hqk,khd->qhd", weights, value_heads, preferred_element_type=jnp.float32)
    return mixed.astype(jnp.bfloat16).reshape(row_count, width)


def body(
    query_rows,
    key_rows,
    value_rows,
    query_norm_gain,
    key_gain,
    break_offset,
    mixer_out_weight,
    routed_tokens,
    expert_gain,
    routes,
    route_scores,
    gate_weight,
    up_weight,
    down_weight,
):
    f32, bf16 = jnp.float32, jnp.bfloat16
    experts = lax.axis_size("ep")
    chips = lax.axis_size("tp") // 2
    my_ep = lax.axis_index("ep")
    core = lax.axis_index("tp") % 2
    count, width = routed_tokens.shape
    half = width // 2
    capacity = count * TOP_K // experts
    slots = experts * capacity

    gates = (gate_weight[0], swap_cores(gate_weight[0]))
    ups = (up_weight[0], swap_cores(up_weight[0]))
    downs = (down_weight[0], swap_cores(down_weight[0]))
    mixers = (mixer_out_weight, swap_cores(mixer_out_weight))

    as_float = routed_tokens.astype(f32)
    normed = (
        as_float
        * lax.rsqrt(jnp.mean(as_float * as_float, axis=1, keepdims=True) + EPS)
        * expert_gain
    ).astype(bf16)
    differences = route_scores[:, None, :] - route_scores[:, :, None]
    route_weight = 1.0 / jnp.sum(jnp.exp(differences), axis=2)

    away = jnp.bitwise_xor(routes, my_ep)
    flat = away.reshape(-1)
    member = (flat[:, None] == jnp.arange(experts, dtype=jnp.int32)[None, :]).astype(bf16)
    earlier = jnp.arange(flat.shape[0])
    earlier = (earlier[None, :] < earlier[:, None]).astype(bf16)
    rank = jnp.dot(earlier, member, preferred_element_type=f32)
    ahead = jnp.sum(rank * member.astype(f32), axis=1).reshape(count, TOP_K)

    weight_high = lax.reduce_precision(route_weight, 8, 7)
    weight_mid = lax.reduce_precision(route_weight - weight_high, 8, 7)
    weight_low = route_weight - weight_high - weight_mid
    tags = jnp.concatenate(
        [away.astype(f32), ahead, weight_high, weight_mid, weight_low], axis=1
    ).astype(bf16)
    tags = jnp.pad(tags, ((0, 0), (0, TAGS - tags.shape[1])))
    tokens = gather_chips(jnp.concatenate([normed[:, half:], tags], axis=1))

    slot_list = jnp.arange(slots, dtype=f32)

    def selection(away_of, ahead_of):
        slot_index = away_of.astype(f32) * capacity + ahead_of
        return (slot_index[..., None] == slot_list).astype(bf16)

    select = selection(away, ahead)
    outgoing = jnp.einsum(
        "ns,nd->sd", jnp.sum(select, axis=1), normed[:, :half], preferred_element_type=f32
    ).astype(bf16).reshape(experts, capacity, half)
    arrived = jnp.stack([outgoing[0]] + [to_distance(outgoing[s], s) for s in range(1, experts)])
    first = gather_chips(arrived).reshape(-1, half)

    away_all = tokens[:, :, half : half + 2].astype(f32)
    ahead_all = tokens[:, :, half + 2 : half + 4].astype(f32)
    weight_all = (
        tokens[:, :, half + 4 : half + 6].astype(f32)
        + tokens[:, :, half + 6 : half + 8].astype(f32)
        + tokens[:, :, half + 8 : half + 10].astype(f32)
    )
    select_all = selection(away_all, ahead_all)
    spread = jnp.einsum(
        "tns,tnd->tsd",
        jnp.sum(select_all, axis=2),
        tokens[:, :, :half],
        preferred_element_type=f32,
    ).astype(bf16).reshape(chips, experts, capacity, half)
    pieces = [spread[:, 0]]
    pieces += [to_distance(spread[:, s], s) for s in range(1, experts)]
    second = jnp.stack(pieces, axis=1).reshape(-1, half)

    heads_mixed = attention(
        query_rows, key_rows, value_rows, query_norm_gain, key_gain, break_offset
    )
    rows = heads_mixed.shape[0] // (2 * chips)
    my_chip = lax.axis_index("tp") // 2
    by_chip = heads_mixed.reshape(chips, 2, rows, -1)
    by_core = jnp.stack(
        [lax.dynamic_index_in_dim(by_chip, (my_chip - d) % chips, 0, keepdims=False) for d in range(chips)]
    )
    mine = lax.dynamic_index_in_dim(by_core, core, 1, keepdims=False)
    theirs = lax.dynamic_index_in_dim(by_core, 1 - core, 1, keepdims=False)
    other = swap_cores(theirs)
    mixer_terms = jnp.dot(
        mine.reshape(chips * rows, -1), mixers[0], preferred_element_type=f32
    ) + jnp.dot(other.reshape(chips * rows, -1), mixers[1], preferred_element_type=f32)
    mixer_terms = mixer_terms.astype(bf16).reshape(chips, 2 * rows, half)

    hidden = []
    for gate, up in zip(gates, ups):
        gate_piece = jnp.dot(first, gate[:half], preferred_element_type=f32) + jnp.dot(
            second, gate[half:], preferred_element_type=f32
        )
        up_piece = jnp.dot(first, up[:half], preferred_element_type=f32) + jnp.dot(
            second, up[half:], preferred_element_type=f32
        )
        hidden.append((jax.nn.silu(gate_piece) * up_piece).astype(bf16))

    def down_terms(columns):
        return (
            jnp.dot(hidden[0], downs[0][:, columns], preferred_element_type=f32)
            + jnp.dot(hidden[1], downs[1][:, columns], preferred_element_type=f32)
        ).astype(bf16).reshape(chips, experts, capacity, half)

    second_terms = down_terms(slice(half, width))
    first_terms = down_terms(slice(0, half))
    first_terms, second_terms = lax.optimization_barrier((first_terms, second_terms))

    first_sum = scatter_chips(first_terms)
    pieces = [second_terms[:, 0]]
    pieces += [to_distance(second_terms[:, s], s) for s in range(1, experts)]
    second_back = jnp.stack(pieces, axis=1).reshape(chips, slots, half)
    picked = jnp.einsum(
        "tnks,tsd->tknd", select_all, second_back, preferred_element_type=f32
    )
    second_mix = jnp.sum(
        jnp.swapaxes(weight_all, 1, 2)[..., None] * picked, axis=1
    ).astype(bf16)
    last_sum = scatter_chips(jnp.concatenate([second_mix, mixer_terms], axis=1))
    first_back = jnp.stack(
        [first_sum[0]] + [to_distance(first_sum[s], s) for s in range(1, experts)]
    ).reshape(slots, half)
    first_picked = jnp.einsum("nks,sd->knd", select, first_back, preferred_element_type=f32)
    first_out = jnp.sum(route_weight.T[..., None] * first_picked, axis=0).astype(bf16)
    expert_output = jnp.concatenate([first_out, last_sum[:count]], axis=1)
    return (last_sum[count:].reshape(rows, width), expert_output)


def solution(mesh):
    in_specs = (
        P("ep", "tp"),
        P("ep", "tp"),
        P("ep", "tp"),
        P(),
        P(),
        P("tp"),
        P("tp", None),
        P(("ep", "tp"), None),
        P(),
        P(("ep", "tp"), None),
        P(("ep", "tp"), None),
        P("ep", None, "tp"),
        P("ep", None, "tp"),
        P("ep", "tp", None),
    )
    out_specs = (P(("ep", "tp"), None), P(("ep", "tp"), None))
    return jax.shard_map(body, mesh=mesh, in_specs=in_specs, out_specs=out_specs, check_vma=False)
```
